1024 devices in a mesh: ep: 64 (over z, y), tp: 16 (over x, core).
Axes of the slice: x: 8, y: 8, z: 8, core: 2. Of those that a mesh axis runs over, the one named last changes fastest.
Arguments:
- tokens: bfloat16 [16384, 2048], P('ep', 'tp'), may hold values from -72 to 72
- norm_gain: bfloat16 [2048], P('tp'), may hold values from 0.099609375 to 1.8984375
- expert_ids: int32 [16384, 2], P('ep'), may hold values from 0 to 63, all different within a row; in each aligned block of 256 rows (0 to 255, 256 to 511, ...) at most 16 rows name the same one
- gate_share: float32 [16384, 2], P('ep'), may hold values from 0.1 to 1
- gate_weight: bfloat16 [64, 2048, 4096], P('ep', None, 'tp'), may hold values from -0.125 to 0.125
- up_weight: bfloat16 [64, 2048, 4096], P('ep', None, 'tp'), may hold values from -0.125 to 0.125
- down_weight: bfloat16 [64, 4096, 2048], P('ep', 'tp'), may hold values from -0.09375 to 0.09375
Outputs:
- mixed: bfloat16 [16384, 2048], P('ep', 'tp')
The draws below stay inside these ranges and needn't reach their ends.
Inputs may be any that keep to these rules, and one draw needn't show every extreme that they name: `expert_ids`: each token names two different experts; among the 256 tokens of one index of ep no expert is named more than 16 times, a bound that some block reaches.
All inputs are finite; a program needn't handle non-finite values.
Results may differ from the reference program's by a relative error of at most 0.019.
Values may be sent and summed in bfloat16 or wider, within the bound.
No kernel may reach another device: no remote copies, remote signals or barrier semaphores. Data moves between devices by JAX's collectives and lax.ppermute only.
A program may use at most 64 MiB of HBM per device.

```python
import math
import jax
import jax.numpy as jnp
import numpy as np
from jax import lax

D = 2048
FF = 4096
TOK_DEV = 256
EXPERTS = 64
CAP = 16
TOKENS = 16384
N_EP = 64
N_TP = 16


def draw_tokens(key, part):
    first, second, third = jax.random.split(key, 3)
    scales = jnp.exp(jax.random.uniform(second, (N_TP,), jnp.float32, jnp.log(0.3), jnp.log(3.0)))
    columns = jnp.repeat(scales, D // N_TP)
    base = jnp.clip(jax.random.normal(first, (TOKENS, D), jnp.float32), -6.0, 6.0)
    return (base * columns[None, :]).astype(jnp.bfloat16)


def levels(rng, extent, pieces, smallest, high):
    def one(dim, shards_of):
        draws = jax.random.uniform(jax.random.fold_in(jax.random.fold_in(rng, 6), dim), (shards_of,), jnp.float32, smallest / len(pieces), high / len(pieces))
        return jnp.repeat(jnp.exp(draws), extent[dim] // shards_of).reshape((-1,) + (1,) * (len(extent) - dim - 1))

    factor_of = one(*pieces[0])
    for cut in pieces[1:]:
        factor_of = factor_of * one(*cut)
    return factor_of


def routed_block(own_key, own, number, rows, count, top, most, skew):
    ranking = jax.random.permutation(own_key, count)
    packed, common = portions_of(count, rows * top, most, skew, True), portions_of(count, rows * top, most, skew, False)
    places = jnp.arange(count)

    def named(lengths, turn):
        used = int((lengths > 0).sum())
        fixed = max(1, used // 4)
        passed = fixed + (places - fixed + turn * (used - fixed)) % max(1, count - fixed)
        return jnp.zeros((count,), jnp.int32).at[ranking[jnp.where(places < fixed, places, passed)]].set(jnp.asarray(lengths, jnp.int32))

    lengths = jnp.where(number % 4 == 0, named(packed, number // 4), named(common, number - number // 4 - 1))
    mixed = jax.random.permutation(jax.random.fold_in(own, 3), count)
    source_of, sink = mixed[0:count // 2 * 2:2], mixed[1:count // 2 * 2:2]
    slack = jnp.minimum(lengths[source_of] - 1, most - lengths[sink]) // 2
    slack = jnp.where((source_of == ranking[0]) | (sink == ranking[0]) | (lengths[sink] == 0), 0, jnp.maximum(slack, 0))
    passed = jax.random.randint(jax.random.fold_in(own, 4), (count // 2,), 0, 1 << 20) % (slack + 1)
    lengths = lengths.at[source_of].add(-passed).at[sink].add(passed)
    members = jnp.searchsorted(jnp.cumsum(lengths), jnp.arange(rows * top), side="right").astype(jnp.int32)
    table = members.reshape(top, rows).T
    table = table[jax.random.permutation(jax.random.fold_in(own, 1), rows)]
    turn = jax.random.randint(jax.random.fold_in(own, 2), (rows, 1), 0, top)
    return jnp.take_along_axis(table, (jnp.arange(top)[None, :] + turn) % top, axis=1)


def portions_of(count, total, limit, skew, full):
    loads = [(1 << 20) // math.isqrt(standing ** skew) + 1 for standing in range(1, count + 1)]
    largest = limit if full else min(limit, max(-(-total // count), total * loads[0] // sum(loads)))
    least = 1 if total - largest >= count - 1 else 0
    given, spare = [largest] + [least] * (count - 1), total - largest - least * (count - 1)
    while spare > 0:
        free = [i for i in range(1, count) if given[i] < largest] or [i for i in range(1, count) if given[i] < limit]
        mass, remaining = sum([loads[i] for i in free]), spare
        for i in free:
            addition = min(limit - given[i], max(1, remaining * loads[i] // mass), spare)
            given[i] = given[i] + addition
            spare = spare - addition
    return np.array(given)


def normal_values(own_key, shape, scale, most, shards=(), kind=jnp.bfloat16):
    result = scale * jax.random.normal(own_key, shape, jnp.float32)
    if shards:
        result = result * levels(own_key, shape, shards, -0.22, 0.18)
    return jnp.clip(result, -most, most).astype(kind)


def setup_inputs(seed: int = 0) -> dict:
    arg_keys = jax.random.split(jax.random.key(seed), 8)
    tokens = draw_tokens(jax.random.fold_in(arg_keys[7], 71), 0)
    norm_gain = jnp.clip(1.0 + 0.18 * jax.random.normal(arg_keys[1], (D,), jnp.float32), 0.099609375, 1.8984375).astype(jnp.bfloat16)
    expert_ids_keys = jax.random.split(jax.random.fold_in(arg_keys[2], 1), TOKENS // TOK_DEV)
    expert_ids_turns = jax.random.permutation(jax.random.fold_in(arg_keys[2], 3), TOKENS // TOK_DEV)
    expert_ids = jax.vmap(lambda own, number: routed_block(jax.random.fold_in(arg_keys[2], 2), own, number, TOK_DEV, EXPERTS, 2, CAP, 2))(expert_ids_keys, expert_ids_turns).reshape((TOKENS, 2))
    gate_share = jnp.clip(0.1 + 0.9 * jax.random.uniform(arg_keys[3], (TOKENS, 2), jnp.float32) ** levels(arg_keys[3], (TOKENS, 2), ((0, 64),), -0.2, 0.2), 0.1, 1.0)
    gate_weight = normal_values(arg_keys[4], (EXPERTS, D, FF), D ** -0.5, 0.125, ((0, 64), (2, 16)))
    up_weight = normal_values(arg_keys[5], (EXPERTS, D, FF), D ** -0.5, 0.125, ((0, 64), (2, 16)))
    down_weight = normal_values(arg_keys[6], (EXPERTS, FF, D), FF ** -0.5, 0.09375, ((0, 64), (1, 16)))
    return {"tokens": tokens, "norm_gain": norm_gain, "expert_ids": expert_ids, "gate_share": gate_share, "gate_weight": gate_weight, "up_weight": up_weight, "down_weight": down_weight}


EPS = 1e-06

def reference(tokens, norm_gain, expert_ids, gate_share, gate_weight, up_weight, down_weight):
    xf = tokens.astype(jnp.float32)
    factor = lax.rsqrt(lax.optimization_barrier(jnp.mean(xf * xf, axis=1, keepdims=True)) + EPS)
    normed = (xf * factor * norm_gain.astype(jnp.float32)[None, :]).astype(jnp.bfloat16)
    blocks = expert_ids.reshape(N_EP, TOK_DEV * 2)
    onehot = (blocks[:, :, None] == jnp.arange(EXPERTS, dtype=jnp.int32)[None, None, :]).astype(jnp.int32)
    slots = lax.optimization_barrier(jnp.sum((jnp.cumsum(onehot, axis=1) - onehot) * onehot, axis=2))
    source = jnp.arange(N_EP, dtype=jnp.int32)[:, None]
    position = (source * CAP + slots).reshape(-1).astype(jnp.int32)
    flat_ids = expert_ids.reshape(-1).astype(jnp.int32)
    rows = jnp.repeat(normed, 2, axis=0)
    buffer = jnp.zeros((EXPERTS, N_EP * CAP, D), jnp.bfloat16).at[flat_ids, position].set(rows)
    width = FF // N_TP

    def expert(args):
        buf, w_gate, w_up, w_down = args
        gate = jnp.dot(buf, w_gate, preferred_element_type=jnp.float32)
        upper = jnp.dot(buf, w_up, preferred_element_type=jnp.float32)
        hidden = (jax.nn.silu(gate) * upper).astype(jnp.bfloat16)

        def add_block(index, total):
            piece = lax.dynamic_slice_in_dim(hidden, index * width, width, 1)
            wpiece = lax.dynamic_slice_in_dim(w_down, index * width, width, 0)
            term = jnp.dot(piece, wpiece, preferred_element_type=jnp.float32).astype(jnp.bfloat16)
            return total + lax.optimization_barrier(term).astype(jnp.float32)
        total = lax.fori_loop(0, N_TP, add_block, jnp.zeros((buf.shape[0], D), jnp.float32))
        return total.astype(jnp.bfloat16)
    outputs = lax.map(expert, (buffer, gate_weight, up_weight, down_weight))
    picked = outputs[flat_ids, position].astype(jnp.float32).reshape(TOKENS, 2, D)
    return lax.optimization_barrier(jnp.sum(picked * gate_share[:, :, None], axis=1)).astype(jnp.bfloat16)
```

```python
import functools

import jax
import jax.numpy as jnp
from jax import lax
from jax.experimental import pallas as pl
from jax.experimental.pallas import tpu as pltpu
from jax.sharding import Mesh, PartitionSpec as P

EPS = 1e-06
PAD = 16
EP = ("z", "y")
X = ("p", "q")
F32 = jnp.float32
BF16 = jnp.bfloat16
INTERPRET = False


def vmem(n):
    return [pl.BlockSpec(memory_space=pltpu.VMEM)] * n


SMEM = pl.BlockSpec(memory_space=pltpu.SMEM)


def call(body, outs, n_in, scalar, flops, name):
    return pl.pallas_call(
        body,
        out_shape=outs,
        in_specs=([SMEM] if scalar else []) + vmem(n_in),
        out_specs=tuple(vmem(len(outs))),
        cost_estimate=pl.CostEstimate(flops=flops, bytes_accessed=4 << 20, transcendentals=0),
        name=name,
        interpret=INTERPRET,
    )


def dispatch_body(experts, core, ids, own, other, buf, rows, gain):
    tok = ids.shape[1]
    half = buf.shape[0] // experts
    e_iota = lax.broadcasted_iota(jnp.int32, (experts, tok), 0)
    hit = [e_iota == ids[k : k + 1, :] for k in range(2)]
    named = (hit[0] | hit[1]).astype(F32).astype(BF16)
    before = lax.broadcasted_iota(jnp.int32, (tok, tok), 0) < lax.broadcasted_iota(
        jnp.int32, (tok, tok), 1
    )
    counts = jnp.dot(named, before.astype(F32).astype(BF16), preferred_element_type=F32)
    first = core[0] * half
    r_iota = lax.broadcasted_iota(jnp.int32, (buf.shape[0], tok), 0)
    place = None
    for k in range(2):
        slot = jnp.sum(jnp.where(hit[k], counts, 0.0), axis=0, keepdims=True).astype(jnp.int32)
        slot = slot - first
        row = jnp.where((slot >= 0) & (slot < half), ids[k : k + 1, :] * half + slot, -1)
        rows[k : k + 1, :] = row
        here = r_iota == row
        place = here if place is None else place | here
    place = place.astype(F32).astype(BF16)
    low = core[0] == 0
    for p in range(own.shape[0]):
        a = own[p]
        b = other[p]
        x = jnp.concatenate([jnp.where(low, a, b), jnp.where(low, b, a)], axis=1)
        buf[:, p * 256 : (p + 1) * 256] = jnp.dot(
            place, x[:tok], preferred_element_type=F32
        ).astype(BF16)
        gain[:, p * 256 : (p + 1) * 256] = x[tok:]


def expert_body(par, mine, gain, other_a, other_b, wg, wu, wd, wg2, wu2, wd2, keep, send_a, send_b):
    q = par[0]
    n = mine.shape[0]
    h = n // 2
    width = 2 * mine.shape[1]
    mine_x = mine[...].astype(F32)
    other_x = jnp.concatenate([other_a[:h], other_b[...]], axis=0).astype(F32)
    squares = jnp.sum(mine_x * mine_x, axis=1, keepdims=True) + jnp.sum(
        other_x * other_x, axis=1, keepdims=True
    )
    factor = lax.rsqrt(squares / width + EPS)
    mine_n = (mine_x * factor * gain[0:1, :].astype(F32)).astype(BF16)
    other_n = (other_x * factor * other_a[h : h + 1, :].astype(F32)).astype(BF16)

    def full(w):
        k = mine.shape[1]
        return jnp.dot(
            mine_n, w[:, pl.ds(q, 1)].reshape(k, w.shape[3]), preferred_element_type=F32
        ) + jnp.dot(
            other_n, w[:, pl.ds(1 - q, 1)].reshape(k, w.shape[3]), preferred_element_type=F32
        )

    def hidden(w_gate, w_up):
        gate = full(w_gate)
        up = full(w_up)
        return (gate / (1.0 + jnp.exp(-gate)) * up).astype(BF16)

    h1 = hidden(wg, wu)
    h2 = hidden(wg2, wu2)
    for p in range(mine.shape[1] // 256):
        cols = slice(p * 256, (p + 1) * 256)
        here = pl.ds(pl.multiple_of(p * 512 + q * 256, 256), 256)
        there = pl.ds(pl.multiple_of(p * 512 + (1 - q) * 256, 256), 256)
        keep[:, cols] = (
            jnp.dot(h1, wd[:, here], preferred_element_type=F32)
            + jnp.dot(h2, wd2[:, here], preferred_element_type=F32)
        ).astype(BF16)
        part = (
            jnp.dot(h1, wd[:, there], preferred_element_type=F32)
            + jnp.dot(h2, wd2[:, there], preferred_element_type=F32)
        ).astype(BF16)
        send_a[:, cols] = part[:h]
        send_b[:, cols] = part[h:]


def add_body(keep, got_a, got_b, out):
    h = got_a.shape[0]
    out[:h] = (keep[:h].astype(F32) + got_a[...].astype(F32)).astype(BF16)
    out[h:] = (keep[h:].astype(F32) + got_b[...].astype(F32)).astype(BF16)


def combine_body(core, rows, share, back, own, other):
    n = back.shape[0]
    tok = rows.shape[1]
    r_iota = lax.broadcasted_iota(jnp.int32, (n, tok), 0)
    weight = jnp.zeros((n, tok), F32)
    for k in range(2):
        weight = jnp.where(r_iota == rows[k : k + 1, :], share[k : k + 1, :], weight)
    high = weight.astype(BF16)
    low = (weight - high.astype(F32)).astype(BF16)
    dims = (((0,), (0,)), ((), ()))
    first = core[0] == 0
    for p in range(own.shape[0]):
        x = back[:, p * 256 : (p + 1) * 256]
        y = lax.dot_general(high, x, dims, preferred_element_type=F32) + lax.dot_general(
            low, x, dims, preferred_element_type=F32
        )
        a = y[:, :128]
        b = y[:, 128:]
        own[p] = jnp.where(first, a, b)
        other[p] = jnp.where(first, b, a)


def shards(tokens, norm_gain, expert_ids, gate_share, gate_weight, up_weight, down_weight):
    tok, width = tokens.shape
    n_ep = lax.axis_size("z") * lax.axis_size("y")
    n_p = lax.axis_size("p")
    slot_cap = 4 * tok // n_ep
    half = slot_cap // 2
    n = n_ep * half
    feats = n_p * 2 * width
    core = lax.axis_index("c").astype(jnp.int32).reshape(1)
    par = lax.axis_index("q").astype(jnp.int32).reshape(1)
    swap = [(0, 1), (1, 0)]
    n_x = 2 * n_p
    beside = [(x, (x + 1) % n_x if x % 2 else (x - 1) % n_x) for x in range(n_x)]

    hid = gate_weight.shape[2]
    wg = gate_weight.reshape(n_p, 2, 256, hid)
    wu = up_weight.reshape(n_p, 2, 256, hid)
    wd = down_weight.reshape(hid, down_weight.shape[2])
    wg2, wu2, wd2 = (lax.ppermute(w, "c", swap) for w in (wg, wu, wd))

    ids = expert_ids.T
    share = gate_share.T
    mine = jnp.concatenate([tokens, jnp.broadcast_to(norm_gain[None, :], (PAD, width))], axis=0)
    gathered = lax.all_gather(mine, "p", axis=0, tiled=False)
    other = lax.ppermute(gathered, "c", swap)
    buf, rows, gain = call(
        functools.partial(dispatch_body, n_ep),
        (
            jax.ShapeDtypeStruct((n, feats), BF16),
            jax.ShapeDtypeStruct((2, tok), jnp.int32),
            jax.ShapeDtypeStruct((PAD, feats), BF16),
        ),
        3,
        True,
        300_000_000,
        "dispatch",
    )(core, ids, gathered, other)
    arrived = lax.all_to_all(
        buf.reshape(n_ep, half, feats), EP, split_axis=0, concat_axis=0, tiled=True
    ).reshape(n, feats)
    h = n // 2
    other_a = lax.ppermute(jnp.concatenate([arrived[:h], gain], axis=0), "q", swap)
    other_b = lax.ppermute(arrived[h:], X, beside)
    piece = jax.ShapeDtypeStruct((h, feats), BF16)
    keep, send_a, send_b = call(
        expert_body,
        (jax.ShapeDtypeStruct((n, feats), BF16), piece, piece),
        10,
        True,
        3_200_000_000,
        "expert",
    )(par, arrived, gain, other_a, other_b, wg, wu, wd, wg2, wu2, wd2)
    got_a = lax.ppermute(send_a, "q", swap)
    got_b = lax.ppermute(send_b, X, beside)
    (sums,) = call(
        add_body, (jax.ShapeDtypeStruct((n, feats), BF16),), 3, False, 1_000_000, "pairsum"
    )(keep, got_a, got_b)
    returned = lax.all_to_all(
        sums.reshape(n_ep, half, feats), EP, split_axis=0, concat_axis=0, tiled=True
    ).reshape(n, feats)
    part = jax.ShapeDtypeStruct((n_p, tok, width), F32)
    own, away = call(combine_body, (part, part), 3, True, 600_000_000, "combine")(
        core, rows, share, returned
    )
    own = (own + lax.ppermute(away, "c", swap)).astype(BF16)
    parts = lax.all_to_all(own, "p", split_axis=0, concat_axis=0, tiled=True)
    return jnp.sum(parts.astype(F32), axis=0).astype(BF16)


def solution(mesh):
    n_ep, n_tp = mesh.devices.shape
    side = 8 if n_ep == 64 else n_ep
    fine = Mesh(
        mesh.devices.reshape(n_ep // side, side, n_tp // 4, 2, 2), ("z", "y", "p", "q", "c")
    )
    tp = ("p", "q", "c")
    in_specs = (
        P(EP, tp),
        P(tp),
        P(EP, None),
        P(EP, None),
        P(EP, None, tp),
        P(EP, None, tp),
        P(EP, tp, None),
    )
    return jax.shard_map(
        shards, mesh=fine, in_specs=in_specs, out_specs=P(EP, tp), check_vma=False
    )
```

```python
import functools

import jax
import jax.numpy as jnp
from jax import lax
from jax.experimental import pallas as pl
from jax.experimental.pallas import tpu as pltpu
from jax.sharding import Mesh, PartitionSpec as P

EPS = 1e-06
PAD = 16
EP = ("z", "y")
X = ("p", "q")
F32 = jnp.float32
BF16 = jnp.bfloat16
INTERPRET = False


def vmem(n):
    return [pl.BlockSpec(memory_space=pltpu.VMEM)] * n


SMEM = pl.BlockSpec(memory_space=pltpu.SMEM)


def call(body, outs, n_in, scalar, flops, name, mib):
    return pl.pallas_call(
        body,
        out_shape=outs,
        in_specs=([SMEM] if scalar else []) + vmem(n_in),
        out_specs=tuple(vmem(len(outs))),
        cost_estimate=pl.CostEstimate(flops=flops, bytes_accessed=4 << 20, transcendentals=0),
        compiler_params=pltpu.CompilerParams(vmem_limit_bytes=mib << 20),
        name=name,
        interpret=INTERPRET,
    )


def dispatch_body(experts, pos, ids, own, other, buf, rows, gain):
    tok = ids.shape[1]
    n_p = own.shape[0]
    half = buf.shape[0] // experts
    core = pos[0]
    e_iota = lax.broadcasted_iota(jnp.int32, (experts, tok), 0)
    hit = [e_iota == ids[k : k + 1, :] for k in range(2)]
    named = (hit[0] | hit[1]).astype(F32).astype(BF16)
    before = lax.broadcasted_iota(jnp.int32, (tok, tok), 0) < lax.broadcasted_iota(
        jnp.int32, (tok, tok), 1
    )
    counts = jnp.dot(named, before.astype(F32).astype(BF16), preferred_element_type=F32)
    r_iota = lax.broadcasted_iota(jnp.int32, (buf.shape[0], tok), 0)
    place = None
    for k in range(2):
        slot = jnp.sum(jnp.where(hit[k], counts, 0.0), axis=0, keepdims=True).astype(jnp.int32)
        slot = slot - core * half
        row = jnp.where((slot >= 0) & (slot < half), ids[k : k + 1, :] * half + slot, -1)
        rows[k : k + 1, :] = row
        here = r_iota == row
        place = here if place is None else place | here
    place = place.astype(F32).astype(BF16)
    low = core == 0
    for s in range(n_p):
        cols = pl.ds(pl.multiple_of(((pos[1] + n_p - s) % n_p) * 256, 256), 256)
        a = own[s]
        b = other[s]
        x = jnp.concatenate([jnp.where(low, a, b), jnp.where(low, b, a)], axis=1)
        buf[:, cols] = jnp.dot(place, x[:tok], preferred_element_type=F32).astype(BF16)
        gain[:, cols] = x[tok:]


def product(x, half, w):
    k = x.shape[1]
    return jnp.dot(x, w[:, pl.ds(half, 1)].reshape(k, w.shape[3]), preferred_element_type=F32)


def near_body(par, mine, gain, wg, wu, wg2, wu2, gate, up, squares):
    x = mine[...].astype(F32)
    squares[...] = jnp.broadcast_to(jnp.sum(x * x, axis=1, keepdims=True), squares.shape)
    y = (x * gain[0:1, :].astype(F32)).astype(BF16)
    hid = wg.shape[3]
    for i, (w_gate, w_up) in enumerate(((wg, wu), (wg2, wu2))):
        cols = slice(i * hid, (i + 1) * hid)
        gate[:, cols] = product(y, par[0], w_gate)
        up[:, cols] = product(y, par[0], w_up)


def far_body(
    par, other_a, other_b, gate, up, squares, wg, wu, wg2, wu2, wd, wd2, send_a, send_b, hidden
):
    h = other_b.shape[0]
    n_in = other_b.shape[1]
    x = jnp.concatenate([other_a[:h], other_b[...]], axis=0).astype(F32)
    total = squares[:, 0:1] + jnp.sum(x * x, axis=1, keepdims=True)
    factor = lax.rsqrt(total / (2 * n_in) + EPS)
    y = (x * other_a[h : h + 1, :].astype(F32)).astype(BF16)
    hid = wg.shape[3]
    half = 1 - par[0]
    for i, (w_gate, w_up) in enumerate(((wg, wu), (wg2, wu2))):
        cols = slice(i * hid, (i + 1) * hid)
        g = (gate[:, cols] + product(y, half, w_gate)) * factor
        u = (up[:, cols] + product(y, half, w_up)) * factor
        hidden[:, cols] = (g / (1.0 + jnp.exp(-g)) * u).astype(BF16)
    down(hidden[...], wd, wd2, half, (send_a, send_b))


def down(hid, wd, wd2, half, outs):
    k = wd.shape[0]
    rows = hid.shape[0] // len(outs)
    for p in range(outs[0].shape[1] // 256):
        cols = pl.ds(pl.multiple_of(p * 512 + half * 256, 256), 256)
        y = (
            jnp.dot(hid[:, :k], wd[:, cols], preferred_element_type=F32)
            + jnp.dot(hid[:, k:], wd2[:, cols], preferred_element_type=F32)
        ).astype(BF16)
        for i, out in enumerate(outs):
            out[:, p * 256 : (p + 1) * 256] = y[i * rows : (i + 1) * rows]


def keep_body(par, hidden, wd, wd2, keep):
    down(hidden[...], wd, wd2, par[0], (keep,))


def add_body(keep, got_a, got_b, out):
    h = got_a.shape[0]
    out[:h] = (keep[:h].astype(F32) + got_a[...].astype(F32)).astype(BF16)
    out[h:] = (keep[h:].astype(F32) + got_b[...].astype(F32)).astype(BF16)


def combine_body(pos, rows, share, back, own, other):
    n = back.shape[0]
    tok = rows.shape[1]
    n_p = own.shape[0]
    r_iota = lax.broadcasted_iota(jnp.int32, (n, tok), 0)
    weight = jnp.zeros((n, tok), F32)
    for k in range(2):
        weight = jnp.where(r_iota == rows[k : k + 1, :], share[k : k + 1, :], weight)
    high = weight.astype(BF16)
    low = (weight - high.astype(F32)).astype(BF16)
    dims = (((0,), (0,)), ((), ()))
    first = pos[0] == 0
    for s in range(n_p):
        x = back[:, pl.ds(pl.multiple_of(((pos[1] + s) % n_p) * 256, 256), 256)]
        y = lax.dot_general(high, x, dims, preferred_element_type=F32) + lax.dot_general(
            low, x, dims, preferred_element_type=F32
        )
        a = y[:, :128]
        b = y[:, 128:]
        own[s] = jnp.where(first, a, b)
        other[s] = jnp.where(first, b, a)


def fold_body(own, got, *outs):
    for s, out in enumerate(outs):
        out[...] = (own[s] + got[s]).astype(BF16)


def shards(tokens, norm_gain, expert_ids, gate_share, gate_weight, up_weight, down_weight):
    tok, width = tokens.shape
    n_ep = lax.axis_size("z") * lax.axis_size("y")
    n_p = lax.axis_size("p")
    slot_cap = 4 * tok // n_ep
    half = slot_cap // 2
    n = n_ep * half
    h = n // 2
    feats = n_p * 2 * width
    pos = jnp.stack([lax.axis_index("c"), lax.axis_index("p")]).astype(jnp.int32)
    par = lax.axis_index("q").astype(jnp.int32).reshape(1)
    swap = [(0, 1), (1, 0)]
    n_x = 2 * n_p
    beside = [(x, (x + 1) % n_x if x % 2 else (x - 1) % n_x) for x in range(n_x)]

    def along(x, s):
        return lax.ppermute(x, "p", [(i, (i + s) % n_p) for i in range(n_p)])

    hid = gate_weight.shape[2]
    wg = gate_weight.reshape(n_p, 2, 256, hid)
    wu = up_weight.reshape(n_p, 2, 256, hid)
    wd = down_weight.reshape(hid, down_weight.shape[2])
    wg2, wu2, wd2 = (lax.ppermute(w, "c", swap) for w in (wg, wu, wd))

    mine = jnp.where(
        lax.broadcasted_iota(jnp.int32, (tok + PAD, width), 0) < tok,
        jnp.pad(tokens, ((0, PAD), (0, 0))),
        norm_gain[None, :],
    )
    gathered = jnp.stack([mine] + [along(mine, s) for s in range(1, n_p)])
    other = lax.ppermute(gathered, "c", swap)

    def shape(*dims, dtype=BF16):
        return jax.ShapeDtypeStruct(dims, dtype)

    buf, rows, gain = call(
        functools.partial(dispatch_body, n_ep),
        (shape(n, feats), shape(2, tok, dtype=jnp.int32), shape(PAD, feats)),
        3,
        True,
        300_000_000,
        "dispatch",
        8,
    )(pos, expert_ids.T, gathered, other)
    arrived = lax.all_to_all(
        buf.reshape(n_ep, half, feats), EP, split_axis=0, concat_axis=0, tiled=True
    ).reshape(n, feats)
    other_a = lax.ppermute(jnp.concatenate([arrived[:h], gain], axis=0), "q", swap)
    other_b = lax.ppermute(arrived[h:], X, beside)
    wide = shape(n, 2 * hid, dtype=F32)
    gate, up, squares = call(
        near_body, (wide, wide, shape(n, 128, dtype=F32)), 6, True, 1_100_000_000, "near", 10
    )(par, arrived, gain, wg, wu, wg2, wu2)
    send_a, send_b, hidden = call(
        far_body,
        (shape(h, feats), shape(h, feats), shape(n, 2 * hid)),
        11,
        True,
        1_600_000_000,
        "far",
        12,
    )(par, other_a, other_b, gate, up, squares, wg, wu, wg2, wu2, wd, wd2)
    got_a = lax.ppermute(send_a, "q", swap)
    got_b = lax.ppermute(send_b, X, beside)
    (keep,) = call(keep_body, (shape(n, feats),), 3, True, 550_000_000, "keep", 6)(
        par, hidden, wd, wd2
    )
    (sums,) = call(add_body, (shape(n, feats),), 3, False, 1_000_000, "pairsum", 4)(
        keep, got_a, got_b
    )
    returned = lax.all_to_all(
        sums.reshape(n_ep, half, feats), EP, split_axis=0, concat_axis=0, tiled=True
    ).reshape(n, feats)
    part = shape(n_p, tok, width, dtype=F32)
    own, away = call(combine_body, (part, part), 3, True, 600_000_000, "combine", 8)(
        pos, rows, gate_share.T, returned
    )
    pieces = call(
        fold_body, (shape(tok, width),) * n_p, 2, False, 1_000_000, "fold", 4
    )(own, lax.ppermute(away, "c", swap))
    total = pieces[0].astype(F32)
    for s in range(1, n_p):
        total = total + along(pieces[s], s).astype(F32)
    return total.astype(BF16)


def solution(mesh):
    n_ep, n_tp = mesh.devices.shape
    side = 8 if n_ep == 64 else n_ep
    fine = Mesh(
        mesh.devices.reshape(n_ep // side, side, n_tp // 4, 2, 2), ("z", "y", "p", "q", "c")
    )
    tp = ("p", "q", "c")
    in_specs = (
        P(EP, tp),
        P(tp),
        P(EP, None),
        P(EP, None),
        P(EP, None, tp),
        P(EP, None, tp),
        P(EP, tp, None),
    )
    return jax.shard_map(
        shards, mesh=fine, in_specs=in_specs, out_specs=P(EP, tp), check_vma=False
    )
```

```python
import functools

import jax
import jax.numpy as jnp
from jax import lax
from jax.experimental import pallas as pl
from jax.experimental.pallas import tpu as pltpu
from jax.sharding import Mesh, PartitionSpec as P

EPS = 1e-06
PAD = 16
EP = ("z", "y")
X = ("g", "r")
TP = ("g", "r", "c")
F32 = jnp.float32
BF16 = jnp.bfloat16
INTERPRET = False


def vmem(n):
    return [pl.BlockSpec(memory_space=pltpu.VMEM)] * n


SMEM = pl.BlockSpec(memory_space=pltpu.SMEM)


def call(body, outs, n_in, scalar, flops, name, mib):
    return pl.pallas_call(
        body,
        out_shape=outs,
        in_specs=([SMEM] if scalar else []) + vmem(n_in),
        out_specs=tuple(vmem(len(outs))),
        cost_estimate=pl.CostEstimate(flops=flops, bytes_accessed=4 << 20, transcendentals=0),
        compiler_params=pltpu.CompilerParams(vmem_limit_bytes=mib << 20),
        name=name,
        interpret=INTERPRET,
    )


def dispatch_body(experts, pos, ids, mine, swapped, far, far_swapped, buf, rows, gain):
    tok = ids.shape[1]
    half = buf.shape[0] // experts
    core = pos[0]
    e_iota = lax.broadcasted_iota(jnp.int32, (experts, tok), 0)
    hit = [e_iota == ids[k : k + 1, :] for k in range(2)]
    named = (hit[0] | hit[1]).astype(F32).astype(BF16)
    before = lax.broadcasted_iota(jnp.int32, (tok, tok), 0) < lax.broadcasted_iota(
        jnp.int32, (tok, tok), 1
    )
    counts = jnp.dot(named, before.astype(F32).astype(BF16), preferred_element_type=F32)
    r_iota = lax.broadcasted_iota(jnp.int32, (buf.shape[0], tok), 0)
    place = None
    for k in range(2):
        slot = jnp.sum(jnp.where(hit[k], counts, 0.0), axis=0, keepdims=True).astype(jnp.int32)
        slot = slot - core * half
        row = jnp.where((slot >= 0) & (slot < half), ids[k : k + 1, :] * half + slot, -1)
        rows[k : k + 1, :] = row
        here = r_iota == row
        place = here if place is None else place | here
    place = place.astype(F32).astype(BF16)
    low = core == 0
    for s, (own, other) in enumerate(((mine, swapped), (far, far_swapped))):
        group = pos[1] if s == 0 else 1 - pos[1]
        cols = pl.ds(pl.multiple_of(group * 256, 256), 256)
        a = own[...]
        b = other[...]
        x = jnp.concatenate([jnp.where(low, a, b), jnp.where(low, b, a)], axis=1)
        buf[:, cols] = jnp.dot(place, x[:tok], preferred_element_type=F32).astype(BF16)
        gain[:, cols] = x[tok:]


def product(x, quarter, w):
    k = x.shape[1]
    return jnp.dot(x, w[:, pl.ds(quarter, 1)].reshape(k, w.shape[3]), preferred_element_type=F32)


def near_body(pos, mine, gain, wg, wu, wg2, wu2, gate, up, squares):
    x = mine[...].astype(F32)
    squares[...] = jnp.broadcast_to(jnp.sum(x * x, axis=1, keepdims=True), squares.shape)
    y = (x * gain[0:1, :].astype(F32)).astype(BF16)
    hid = wg.shape[3]
    for i, (w_gate, w_up) in enumerate(((wg, wu), (wg2, wu2))):
        cols = slice(i * hid, (i + 1) * hid)
        gate[:, cols] = product(y, pos[2], w_gate)
        up[:, cols] = product(y, pos[2], w_up)


def middle_body(
    pos, left, right, gain_l, gain_r, gate_in, up_in, squares_in, wg, wu, wg2, wu2, gate, up, squares
):
    total = squares_in[...]
    ys = []
    for piece, gain in ((left, gain_l), (right, gain_r)):
        x = piece[...].astype(F32)
        total = total + jnp.sum(x * x, axis=1, keepdims=True)
        ys.append((x * gain[0:1, :].astype(F32)).astype(BF16))
    squares[...] = total
    ql = (pos[2] + 3) % 4
    qr = (pos[2] + 1) % 4
    hid = wg.shape[3]
    for i, (w_gate, w_up) in enumerate(((wg, wu), (wg2, wu2))):
        cols = slice(i * hid, (i + 1) * hid)
        gate[:, cols] = gate_in[:, cols] + (product(ys[0], ql, w_gate) + product(ys[1], qr, w_gate))
        up[:, cols] = up_in[:, cols] + (product(ys[0], ql, w_up) + product(ys[1], qr, w_up))


def far_body(
    pos, left2, right2, gain, gate, up, squares, wg, wu, wg2, wu2, wd, wd2, send_a, send_b, hidden
):
    x = jnp.concatenate([left2[...], right2[...]], axis=0).astype(F32)
    total = squares[:, 0:1] + jnp.sum(x * x, axis=1, keepdims=True)
    factor = lax.rsqrt(total / (4 * x.shape[1]) + EPS)
    y = (x * gain[0:1, :].astype(F32)).astype(BF16)
    hid = wg.shape[3]
    quarter = (pos[2] + 2) % 4
    for i, (w_gate, w_up) in enumerate(((wg, wu), (wg2, wu2))):
        cols = slice(i * hid, (i + 1) * hid)
        g = (gate[:, cols] + product(y, quarter, w_gate)) * factor
        u = (up[:, cols] + product(y, quarter, w_up)) * factor
        hidden[:, cols] = (g / (1.0 + jnp.exp(-g)) * u).astype(BF16)
    down(hidden[...], wd, wd2, quarter, (send_a, send_b))


def down(hid, wd, wd2, quarter, outs):
    k = wd.shape[0]
    rows = hid.shape[0] // len(outs)
    for g in range(2):
        cols = pl.ds(pl.multiple_of(g * 1024 + quarter * 256, 256), 256)
        y = (
            jnp.dot(hid[:, :k], wd[:, cols], preferred_element_type=F32)
            + jnp.dot(hid[:, k:], wd2[:, cols], preferred_element_type=F32)
        ).astype(BF16)
        for i, out in enumerate(outs):
            out[:, g * 256 : (g + 1) * 256] = y[i * rows : (i + 1) * rows]


def keep_body(pos, hidden, wd, wd2, to_left, keep, to_right):
    hid = hidden[...]
    down(hid, wd, wd2, (pos[2] + 3) % 4, (to_left,))
    down(hid, wd, wd2, pos[2], (keep,))
    down(hid, wd, wd2, (pos[2] + 1) % 4, (to_right,))


def relay_body(to_left, to_right, got_a, got_b, left, right):
    h = got_a.shape[0]
    right[:h] = (to_right[:h].astype(F32) + got_a[...].astype(F32)).astype(BF16)
    right[h:] = to_right[h:]
    left[:h] = to_left[:h]
    left[h:] = (to_left[h:].astype(F32) + got_b[...].astype(F32)).astype(BF16)


def add_body(keep, got_a, got_b, out):
    out[...] = (
        keep[...].astype(F32) + got_a[...].astype(F32) + got_b[...].astype(F32)
    ).astype(BF16)


def combine_body(pos, rows, share, back, own, swapped, far, far_swapped):
    n = back.shape[0]
    tok = rows.shape[1]
    r_iota = lax.broadcasted_iota(jnp.int32, (n, tok), 0)
    weight = jnp.zeros((n, tok), F32)
    for k in range(2):
        weight = jnp.where(r_iota == rows[k : k + 1, :], share[k : k + 1, :], weight)
    high = weight.astype(BF16)
    low = (weight - high.astype(F32)).astype(BF16)
    dims = (((0,), (0,)), ((), ()))
    first = pos[0] == 0
    for s, (mine, other) in enumerate(((own, swapped), (far, far_swapped))):
        group = pos[1] if s == 0 else 1 - pos[1]
        x = back[:, pl.ds(pl.multiple_of(group * 256, 256), 256)]
        y = lax.dot_general(high, x, dims, preferred_element_type=F32) + lax.dot_general(
            low, x, dims, preferred_element_type=F32
        )
        a = y[:, :128]
        b = y[:, 128:]
        mine[...] = jnp.where(first, a, b).astype(mine.dtype)
        other[...] = jnp.where(first, b, a).astype(other.dtype)


def shards(tokens, norm_gain, expert_ids, gate_share, gate_weight, up_weight, down_weight):
    tok, width = tokens.shape
    n_ep = lax.axis_size("z") * lax.axis_size("y")
    slot_cap = 4 * tok // n_ep
    half = slot_cap // 2
    n = n_ep * half
    h = n // 2
    feats = 4 * width
    pos = jnp.stack([lax.axis_index("c"), lax.axis_index("g"), lax.axis_index("r")])
    pos = pos.astype(jnp.int32)
    swap = [(0, 1), (1, 0)]

    def step(x, s):
        return lax.ppermute(x, X, [(i, (i + s) % 8) for i in range(8)])

    def flip(x, bits):
        return lax.ppermute(x, TP, [(i, i ^ bits) for i in range(16)])

    hid = gate_weight.shape[2]
    wg = gate_weight.reshape(2, 4, 256, hid)
    wu = up_weight.reshape(2, 4, 256, hid)
    wd = down_weight.reshape(hid, down_weight.shape[2])
    wg2, wu2, wd2 = (lax.ppermute(w, "c", swap) for w in (wg, wu, wd))

    mine = jnp.where(
        lax.broadcasted_iota(jnp.int32, (tok + PAD, width), 0) < tok,
        jnp.pad(tokens, ((0, PAD), (0, 0))),
        norm_gain[None, :],
    )
    far, far_swapped, swapped = flip(mine, 8), flip(mine, 9), flip(mine, 1)

    def shape(*dims, dtype=BF16):
        return jax.ShapeDtypeStruct(dims, dtype)

    buf, rows, gain = call(
        functools.partial(dispatch_body, n_ep),
        (shape(n, feats), shape(2, tok, dtype=jnp.int32), shape(PAD, feats)),
        5,
        True,
        150_000_000,
        "dispatch",
        8,
    )(pos, expert_ids.T, mine, swapped, far, far_swapped)
    gain_l, gain_r, gain_2 = step(gain, 1), step(gain, -1), step(gain, 2)
    here = lax.all_to_all(
        buf.reshape(n_ep, half, feats), EP, split_axis=0, concat_axis=0, tiled=True
    ).reshape(n, feats)
    here, gain_l, gain_r, gain_2 = lax.optimization_barrier((here, gain_l, gain_r, gain_2))
    wide = shape(n, 2 * hid, dtype=F32)
    thin = shape(n, 128, dtype=F32)
    left = step(here, 1)
    right = step(here, -1)
    gate, up, squares = call(near_body, (wide, wide, thin), 6, True, 600_000_000, "near", 8)(
        pos, here, gain, wg, wu, wg2, wu2
    )
    left2 = step(left[:h], 1)
    right2 = step(right[h:], -1)
    gate, up, squares = call(
        middle_body, (wide, wide, thin), 11, True, 1_100_000_000, "middle", 10
    )(pos, left, right, gain_l, gain_r, gate, up, squares, wg, wu, wg2, wu2)
    send_a, send_b, hidden = call(
        far_body,
        (shape(h, feats), shape(h, feats), shape(n, 2 * hid)),
        12,
        True,
        800_000_000,
        "far",
        10,
    )(pos, left2, right2, gain_2, gate, up, squares, wg, wu, wg2, wu2, wd, wd2)
    got_a = step(send_a, 1)
    got_b = step(send_b, -1)
    whole = shape(n, feats)
    to_left, keep, to_right = call(
        keep_body, (whole, whole, whole), 3, True, 800_000_000, "keep", 6
    )(pos, hidden, wd, wd2)
    to_left, to_right = call(relay_body, (whole, whole), 4, False, 1_000_000, "relay", 4)(
        to_left, to_right, got_a, got_b
    )
    from_left = step(to_right, 1)
    from_right = step(to_left, -1)
    (sums,) = call(add_body, (whole,), 3, False, 1_000_000, "pairsum", 4)(
        keep, from_left, from_right
    )
    returned = lax.all_to_all(
        sums.reshape(n_ep, half, feats), EP, split_axis=0, concat_axis=0, tiled=True
    ).reshape(n, feats)
    part = shape(tok, width, dtype=F32)
    sent = shape(tok, width)
    own, swapped, far, far_swapped = call(
        combine_body, (part, part, sent, sent), 3, True, 300_000_000, "combine", 8
    )(pos, rows, gate_share.T, returned)
    total = own + flip(far, 8).astype(F32) + flip(far_swapped, 9).astype(F32) + flip(swapped, 1)
    return total.astype(BF16)


def solution(mesh):
    n_ep, n_tp = mesh.devices.shape
    side = 8 if n_ep == 64 else n_ep
    fine = Mesh(
        mesh.devices.reshape(n_ep // side, side, 2, n_tp // 4, 2), ("z", "y", "g", "r", "c")
    )
    tp = TP
    in_specs = (
        P(EP, tp),
        P(tp),
        P(EP, None),
        P(EP, None),
        P(EP, None, tp),
        P(EP, None, tp),
        P(EP, tp, None),
    )
    return jax.shard_map(
        shards, mesh=fine, in_specs=in_specs, out_specs=P(EP, tp), check_vma=False
    )
```

```python
import functools

import jax
import jax.numpy as jnp
from jax import lax
from jax.experimental import pallas as pl
from jax.experimental.pallas import tpu as pltpu
from jax.sharding import Mesh, PartitionSpec as P

EPS = 1e-06
PAD = 16
EP = ("z", "y")
X = ("g", "r")
TP = ("g", "r", "c")
F32 = jnp.float32
BF16 = jnp.bfloat16
INTERPRET = False


def vmem(n):
    return [pl.BlockSpec(memory_space=pltpu.VMEM)] * n


SMEM = pl.BlockSpec(memory_space=pltpu.SMEM)


def call(body, outs, n_in, scalar, flops, mib):
    return pl.pallas_call(
        body,
        out_shape=outs,
        in_specs=([SMEM] if scalar else []) + vmem(n_in),
        out_specs=tuple(vmem(len(outs))),
        cost_estimate=pl.CostEstimate(flops=flops, bytes_accessed=4 << 20, transcendentals=0),
        compiler_params=pltpu.CompilerParams(vmem_limit_bytes=mib << 20),
        interpret=INTERPRET,
    )


def slots_body(experts, pos, ids, rows, place):
    tok = ids.shape[1]
    half = place.shape[0] // experts
    e_iota = lax.broadcasted_iota(jnp.int32, (experts, tok), 0)
    hit = [e_iota == ids[k : k + 1, :] for k in range(2)]
    named = (hit[0] | hit[1]).astype(F32).astype(BF16)
    before = lax.broadcasted_iota(jnp.int32, (tok, tok), 0) < lax.broadcasted_iota(
        jnp.int32, (tok, tok), 1
    )
    counts = jnp.dot(named, before.astype(F32).astype(BF16), preferred_element_type=F32)
    r_iota = lax.broadcasted_iota(jnp.int32, place.shape, 0)
    here = None
    for k in range(2):
        slot = jnp.sum(jnp.where(hit[k], counts, 0.0), axis=0, keepdims=True).astype(jnp.int32)
        slot = slot - pos[0] * half
        row = jnp.where((slot >= 0) & (slot < half), ids[k : k + 1, :] * half + slot, -1)
        rows[k : k + 1, :] = row
        match = r_iota == row
        here = match if here is None else here | match
    place[...] = here.astype(F32).astype(BF16)


def dispatch_body(pos, place, own, other, buf, gain):
    tok = place.shape[1]
    low = pos[0] == 0
    for s in range(2):
        group = pos[1] if s == 0 else 1 - pos[1]
        cols = pl.ds(pl.multiple_of(group * 256, 256), 256)
        a = own[s]
        b = other[s]
        x = jnp.concatenate([jnp.where(low, a, b), jnp.where(low, b, a)], axis=1)
        buf[:, cols] = jnp.dot(place[...], x[:tok], preferred_element_type=F32).astype(BF16)
        gain[:, cols] = x[tok:]


def product(x, quarter, w):
    k = x.shape[1]
    return jnp.dot(x, w[:, pl.ds(quarter, 1)].reshape(k, w.shape[3]), preferred_element_type=F32)


def near_body(pos, mine, gain, wg, wu, gate, up, squares):
    x = mine[...].astype(F32)
    squares[...] = jnp.broadcast_to(jnp.sum(x * x, axis=1, keepdims=True), squares.shape)
    y = (x * gain[0:1, :].astype(F32)).astype(BF16)
    gate[...] = product(y, pos[2], wg)
    up[...] = product(y, pos[2], wu)


def middle_body(
    pos, mine, gain_m, left, right, gate_in, up_in, squares_in, wg, wu, wg2, wu2, gate, up, squares
):
    n = mine.shape[0]
    total = squares_in[...]
    ys = []
    for piece in (left, right):
        x = piece[:n].astype(F32)
        total = total + jnp.sum(x * x, axis=1, keepdims=True)
        ys.append((x * piece[n : n + 1, :].astype(F32)).astype(BF16))
    squares[...] = total
    y = (mine[...].astype(F32) * gain_m[0:1, :].astype(F32)).astype(BF16)
    ql = (pos[2] + 3) % 4
    qr = (pos[2] + 1) % 4
    hid = wg.shape[3]
    for w, start, out in ((wg, gate_in, gate), (wu, up_in, up)):
        out[:, :hid] = start[...] + (product(ys[0], ql, w) + product(ys[1], qr, w))
    for w, out in ((wg2, gate), (wu2, up)):
        out[:, hid:] = product(y, pos[2], w) + (product(ys[0], ql, w) + product(ys[1], qr, w))


def far_body(
    pos, left2, right2, gate, up, squares, wg, wu, wg2, wu2, wd, wd2, send_a, send_b, hidden
):
    h = left2.shape[0]
    x = jnp.concatenate([left2[...], right2[:h]], axis=0).astype(F32)
    total = squares[:, 0:1] + jnp.sum(x * x, axis=1, keepdims=True)
    factor = lax.rsqrt(total / (4 * x.shape[1]) + EPS)
    y = (x * right2[h : h + 1, :].astype(F32)).astype(BF16)
    hid = wg.shape[3]
    quarter = (pos[2] + 2) % 4
    for i, (w_gate, w_up) in enumerate(((wg, wu), (wg2, wu2))):
        cols = slice(i * hid, (i + 1) * hid)
        g = (gate[:, cols] + product(y, quarter, w_gate)) * factor
        u = (up[:, cols] + product(y, quarter, w_up)) * factor
        hidden[:, cols] = (g / (1.0 + jnp.exp(-g)) * u).astype(BF16)
    down(hidden[...], wd, wd2, quarter, (send_a, send_b))


def down(hid, wd, wd2, quarter, outs):
    k = wd.shape[0]
    rows = hid.shape[0] // len(outs)
    for g in range(2):
        cols = pl.ds(pl.multiple_of(g * 1024 + quarter * 256, 256), 256)
        y = (
            jnp.dot(hid[:, :k], wd[:, cols], preferred_element_type=F32)
            + jnp.dot(hid[:, k:], wd2[:, cols], preferred_element_type=F32)
        ).astype(BF16)
        for i, out in enumerate(outs):
            out[:, g * 256 : (g + 1) * 256] = y[i * rows : (i + 1) * rows]


def keep_body(pos, hidden, wd, wd2, to_left, keep, to_right):
    hid = hidden[...]
    down(hid, wd, wd2, (pos[2] + 3) % 4, (to_left,))
    down(hid, wd, wd2, pos[2], (keep,))
    down(hid, wd, wd2, (pos[2] + 1) % 4, (to_right,))


def relay_body(to_left, to_right, got_a, got_b, left, right):
    h = got_a.shape[0]
    right[:h] = (to_right[:h].astype(F32) + got_a[...].astype(F32)).astype(BF16)
    right[h:] = to_right[h:]
    left[:h] = to_left[:h]
    left[h:] = (to_left[h:].astype(F32) + got_b[...].astype(F32)).astype(BF16)


def add_body(keep, got_a, got_b, out):
    out[...] = (
        keep[...].astype(F32) + got_a[...].astype(F32) + got_b[...].astype(F32)
    ).astype(BF16)


def mix_body(rows, share, high, low):
    r_iota = lax.broadcasted_iota(jnp.int32, high.shape, 0)
    weight = jnp.zeros(high.shape, F32)
    for k in range(2):
        weight = jnp.where(r_iota == rows[k : k + 1, :], share[k : k + 1, :], weight)
    top = weight.astype(BF16)
    high[...] = top
    low[...] = (weight - top.astype(F32)).astype(BF16)


def combine_body(pos, high, low, back, near, near_away, far, far_away):
    dims = (((0,), (0,)), ((), ()))
    first = pos[0] == 0
    for s, (mine, other) in enumerate(((near, near_away), (far, far_away))):
        group = pos[1] if s == 0 else 1 - pos[1]
        x = back[:, pl.ds(pl.multiple_of(group * 256, 256), 256)]
        y = lax.dot_general(high[...], x, dims, preferred_element_type=F32) + lax.dot_general(
            low[...], x, dims, preferred_element_type=F32
        )
        a = y[:, :128]
        b = y[:, 128:]
        mine[...] = jnp.where(first, a, b)
        other[...] = jnp.where(first, b, a)


def fold_body(own, got, out):
    out[...] = (own[...] + got[...]).astype(BF16)


def shards(tokens, norm_gain, expert_ids, gate_share, gate_weight, up_weight, down_weight):
    tok, width = tokens.shape
    n_ep = lax.axis_size("z") * lax.axis_size("y")
    slot_cap = 4 * tok // n_ep
    half = slot_cap // 2
    n = n_ep * half
    h = n // 2
    feats = 4 * width
    pos = jnp.stack([lax.axis_index("c"), lax.axis_index("g"), lax.axis_index("r")])
    pos = pos.astype(jnp.int32)

    def step(x, s):
        return lax.ppermute(x, X, [(i, (i + s) % 8) for i in range(8)])

    def flip(x, bits):
        return lax.ppermute(x, TP, [(i, i ^ bits) for i in range(16)])

    hid = gate_weight.shape[2]
    wg = gate_weight.reshape(2, 4, 256, hid)
    wu = up_weight.reshape(2, 4, 256, hid)
    wd = down_weight.reshape(hid, down_weight.shape[2])

    def shape(*dims, dtype=BF16):
        return jax.ShapeDtypeStruct(dims, dtype)

    rows, place = call(
        functools.partial(slots_body, n_ep),
        (shape(2, tok, dtype=jnp.int32), shape(n, tok)),
        1,
        True,
        20_000_000,
        4,
    )(pos, expert_ids.T)
    mine = jnp.where(
        lax.broadcasted_iota(jnp.int32, (tok + PAD, width), 0) < tok,
        jnp.pad(tokens, ((0, PAD), (0, 0))),
        norm_gain[None, :],
    )
    own = jnp.stack([mine, flip(mine, 8)])
    other = flip(own, 1)
    buf, gain = call(
        dispatch_body, (shape(n, feats), shape(PAD, feats)), 3, True, 150_000_000, 4
    )(pos, place, own, other)
    here = lax.all_to_all(
        buf.reshape(n_ep, half, feats), EP, split_axis=0, concat_axis=0, tiled=True
    ).reshape(n, feats)
    sent = jnp.concatenate([here, gain], axis=0)
    left = step(sent, 1)
    right = step(sent, -1)
    wg2, wu2, wd2 = flip(wg, 1), flip(wu, 1), flip(wd, 1)
    wide = shape(n, 2 * hid, dtype=F32)
    slim = shape(n, hid, dtype=F32)
    thin = shape(n, 128, dtype=F32)
    gate, up, squares = call(near_body, (slim, slim, thin), 4, True, 300_000_000, 6)(
        pos, here, gain, wg, wu
    )
    left, right, gate = lax.optimization_barrier((left, right, gate))
    left2 = step(left[:h], 1)
    right2 = step(right[h:], -1)
    gate, up, squares = call(
        middle_body, (wide, wide, thin), 11, True, 1_300_000_000, 10
    )(pos, here, gain, left, right, gate, up, squares, wg, wu, wg2, wu2)
    send_a, send_b, hidden = call(
        far_body, (shape(h, feats), shape(h, feats), shape(n, 2 * hid)), 11, True, 800_000_000, 10
    )(pos, left2, right2, gate, up, squares, wg, wu, wg2, wu2, wd, wd2)
    got_a = step(send_a, 1)
    got_b = step(send_b, -1)
    whole = shape(n, feats)
    to_left, keep, to_right = call(
        keep_body, (whole, whole, whole), 3, True, 800_000_000, 6
    )(pos, hidden, wd, wd2)
    to_left, to_right = call(relay_body, (whole, whole), 4, False, 1_000_000, 4)(
        to_left, to_right, got_a, got_b
    )
    from_left = step(to_right, 1)
    from_right = step(to_left, -1)
    (sums,) = call(add_body, (whole,), 3, False, 1_000_000, 4)(keep, from_left, from_right)
    returned = lax.all_to_all(
        sums.reshape(n_ep, half, feats), EP, split_axis=0, concat_axis=0, tiled=True
    ).reshape(n, feats)
    high, low = call(mix_body, (shape(n, tok), shape(n, tok)), 2, False, 1_000_000, 4)(
        rows, gate_share.T
    )
    part = shape(tok, width, dtype=F32)
    near, near_away, far, far_away = call(
        combine_body, (part, part, part, part), 3, True, 300_000_000, 6
    )(pos, high, low, returned)
    (folded,) = call(fold_body, (shape(tok, width),), 2, False, 1_000_000, 2)(
        far, flip(far_away, 1)
    )
    return (near + flip(near_away, 1) + flip(folded, 8).astype(F32)).astype(BF16)


def solution(mesh):
    n_ep, n_tp = mesh.devices.shape
    side = 8 if n_ep == 64 else n_ep
    fine = Mesh(
        mesh.devices.reshape(n_ep // side, side, 2, n_tp // 4, 2), ("z", "y", "g", "r", "c")
    )
    tp = TP
    in_specs = (
        P(EP, tp),
        P(tp),
        P(EP, None),
        P(EP, None),
        P(EP, None, tp),
        P(EP, None, tp),
        P(EP, tp, None),
    )
    return jax.shard_map(shards, mesh=fine, in_specs=in_specs, out_specs=P(EP, tp), check_vma=False)
```

```python
import functools

import jax
import jax.numpy as jnp
from jax import lax
from jax.experimental import pallas as pl
from jax.experimental.pallas import tpu as pltpu
from jax.sharding import Mesh, PartitionSpec as P

EPS = 1e-06
PAD = 16
EP = ("z", "y")
X = ("g", "r")
TP = ("g", "r", "c")
F32 = jnp.float32
BF16 = jnp.bfloat16
INTERPRET = False


def vmem(n):
    return [pl.BlockSpec(memory_space=pltpu.VMEM)] * n


SMEM = pl.BlockSpec(memory_space=pltpu.SMEM)


def call(body, outs, n_in, scalar, flops, mib):
    return pl.pallas_call(
        body,
        out_shape=outs,
        in_specs=([SMEM] if scalar else []) + vmem(n_in),
        out_specs=tuple(vmem(len(outs))),
        cost_estimate=pl.CostEstimate(flops=flops, bytes_accessed=4 << 20, transcendentals=0),
        compiler_params=pltpu.CompilerParams(vmem_limit_bytes=mib << 20),
        interpret=INTERPRET,
    )


def slots_body(experts, pos, ids, rows, place):
    tok = ids.shape[1]
    half = place.shape[0] // experts
    e_iota = lax.broadcasted_iota(jnp.int32, (experts, tok), 0)
    hit = [e_iota == ids[k : k + 1, :] for k in range(2)]
    named = (hit[0] | hit[1]).astype(F32).astype(BF16)
    before = lax.broadcasted_iota(jnp.int32, (tok, tok), 0) < lax.broadcasted_iota(
        jnp.int32, (tok, tok), 1
    )
    counts = jnp.dot(named, before.astype(F32).astype(BF16), preferred_element_type=F32)
    r_iota = lax.broadcasted_iota(jnp.int32, place.shape, 0)
    here = None
    for k in range(2):
        slot = jnp.sum(jnp.where(hit[k], counts, 0.0), axis=0, keepdims=True).astype(jnp.int32)
        slot = slot - pos[0] * half
        row = jnp.where((slot >= 0) & (slot < half), ids[k : k + 1, :] * half + slot, -1)
        rows[k : k + 1, :] = row
        match = r_iota == row
        here = match if here is None else here | match
    place[...] = here.astype(F32).astype(BF16)


def dispatch_body(pos, place, own, other, buf, gain):
    tok = place.shape[1]
    low = pos[0] == 0
    for s in range(2):
        group = pos[1] if s == 0 else 1 - pos[1]
        cols = pl.ds(pl.multiple_of(group * 256, 256), 256)
        a = own[s]
        b = other[s]
        x = jnp.concatenate([jnp.where(low, a, b), jnp.where(low, b, a)], axis=1)
        buf[:, cols] = jnp.dot(place[...], x[:tok], preferred_element_type=F32).astype(BF16)
        gain[:, cols] = x[tok:]


def product(x, quarter, w):
    k = x.shape[1]
    return jnp.dot(x, w[:, pl.ds(quarter, 1)].reshape(k, w.shape[3]), preferred_element_type=F32)


def near_body(pos, mine, gain, wg, wu, gate, up, squares):
    x = mine[...].astype(F32)
    squares[...] = jnp.broadcast_to(jnp.sum(x * x, axis=1, keepdims=True), squares.shape)
    y = (x * gain[0:1, :].astype(F32)).astype(BF16)
    gate[...] = product(y, pos[2], wg)
    up[...] = product(y, pos[2], wu)


def middle_body(
    pos, mine, gain_m, left, right, gate_in, up_in, squares_in, wg, wu, wg2, wu2, gate, up, squares
):
    n = mine.shape[0]
    total = squares_in[...]
    ys = []
    for piece in (left, right):
        x = piece[:n].astype(F32)
        total = total + jnp.sum(x * x, axis=1, keepdims=True)
        ys.append((x * piece[n : n + 1, :].astype(F32)).astype(BF16))
    squares[...] = total
    y = (mine[...].astype(F32) * gain_m[0:1, :].astype(F32)).astype(BF16)
    ql = (pos[2] + 3) % 4
    qr = (pos[2] + 1) % 4
    hid = wg.shape[3]
    for w, start, out in ((wg, gate_in, gate), (wu, up_in, up)):
        out[:, :hid] = start[...] + (product(ys[0], ql, w) + product(ys[1], qr, w))
    for w, out in ((wg2, gate), (wu2, up)):
        out[:, hid:] = product(y, pos[2], w) + (product(ys[0], ql, w) + product(ys[1], qr, w))


def far_body(
    pos, left2, right2, gate, up, squares, wg, wu, wg2, wu2, wd, wd2, send_a, send_b, hidden
):
    h = left2.shape[0]
    x = jnp.concatenate([left2[...], right2[:h]], axis=0).astype(F32)
    total = squares[:, 0:1] + jnp.sum(x * x, axis=1, keepdims=True)
    factor = lax.rsqrt(total / (4 * x.shape[1]) + EPS)
    y = (x * right2[h : h + 1, :].astype(F32)).astype(BF16)
    hid = wg.shape[3]
    quarter = (pos[2] + 2) % 4
    for i, (w_gate, w_up) in enumerate(((wg, wu), (wg2, wu2))):
        cols = slice(i * hid, (i + 1) * hid)
        g = (gate[:, cols] + product(y, quarter, w_gate)) * factor
        u = (up[:, cols] + product(y, quarter, w_up)) * factor
        hidden[:, cols] = (g / (1.0 + jnp.exp(-g)) * u).astype(BF16)
    down(hidden[...], wd, wd2, quarter, (send_a, send_b))


def down(hid, wd, wd2, quarter, outs):
    k = wd.shape[0]
    rows = hid.shape[0] // len(outs)
    for g in range(2):
        cols = pl.ds(pl.multiple_of(g * 1024 + quarter * 256, 256), 256)
        y = (
            jnp.dot(hid[:, :k], wd[:, cols], preferred_element_type=F32)
            + jnp.dot(hid[:, k:], wd2[:, cols], preferred_element_type=F32)
        ).astype(BF16)
        for i, out in enumerate(outs):
            out[:, g * 256 : (g + 1) * 256] = y[i * rows : (i + 1) * rows]


def keep_body(pos, hidden, wd, wd2, to_left, keep, to_right):
    hid = hidden[...]
    down(hid, wd, wd2, (pos[2] + 3) % 4, (to_left,))
    down(hid, wd, wd2, pos[2], (keep,))
    down(hid, wd, wd2, (pos[2] + 1) % 4, (to_right,))


def relay_body(to_left, to_right, got_a, got_b, left, right):
    h = got_a.shape[0]
    right[:h] = (to_right[:h].astype(F32) + got_a[...].astype(F32)).astype(BF16)
    right[h:] = to_right[h:]
    left[:h] = to_left[:h]
    left[h:] = (to_left[h:].astype(F32) + got_b[...].astype(F32)).astype(BF16)


def add_body(keep, got_a, got_b, out):
    out[...] = (
        keep[...].astype(F32) + got_a[...].astype(F32) + got_b[...].astype(F32)
    ).astype(BF16)


def mix_body(part, rows, share, out):
    r_iota = lax.broadcasted_iota(jnp.int32, out.shape, 0)
    weight = jnp.zeros(out.shape, F32)
    for k in range(2):
        weight = jnp.where(r_iota == rows[k : k + 1, :], share[k : k + 1, :], weight)
    top = weight.astype(BF16)
    out[...] = top if part == 0 else (weight - top.astype(F32)).astype(BF16)


def combine_body(pos, high, low, back, own, away):
    dims = (((0,), (0,)), ((), ()))
    first = pos[0] == 0
    for s in range(2):
        group = pos[1] if s == 0 else 1 - pos[1]
        x = back[:, pl.ds(pl.multiple_of(group * 256, 256), 256)]
        y = lax.dot_general(high[...], x, dims, preferred_element_type=F32) + lax.dot_general(
            low[...], x, dims, preferred_element_type=F32
        )
        a = y[:, :128]
        b = y[:, 128:]
        own[s] = jnp.where(first, a, b)
        away[s] = jnp.where(first, b, a)


def fold_body(own, got, near, far):
    far[...] = (own[1] + got[1]).astype(BF16)
    near[...] = own[0] + got[0]


def shards(tokens, norm_gain, expert_ids, gate_share, gate_weight, up_weight, down_weight):
    tok, width = tokens.shape
    n_ep = lax.axis_size("z") * lax.axis_size("y")
    slot_cap = 4 * tok // n_ep
    half = slot_cap // 2
    n = n_ep * half
    h = n // 2
    feats = 4 * width
    pos = jnp.stack([lax.axis_index("c"), lax.axis_index("g"), lax.axis_index("r")])
    pos = pos.astype(jnp.int32)

    def step(x, s):
        return lax.ppermute(x, X, [(i, (i + s) % 8) for i in range(8)])

    def flip(x, bits):
        return lax.ppermute(x, TP, [(i, i ^ bits) for i in range(16)])

    hid = gate_weight.shape[2]
    wg = gate_weight.reshape(2, 4, 256, hid)
    wu = up_weight.reshape(2, 4, 256, hid)
    wd = down_weight.reshape(hid, down_weight.shape[2])

    def shape(*dims, dtype=BF16):
        return jax.ShapeDtypeStruct(dims, dtype)

    rows, place = call(
        functools.partial(slots_body, n_ep),
        (shape(2, tok, dtype=jnp.int32), shape(n, tok)),
        1,
        True,
        20_000_000,
        4,
    )(pos, expert_ids.T)
    mine = jnp.where(
        lax.broadcasted_iota(jnp.int32, (tok + PAD, width), 0) < tok,
        jnp.pad(tokens, ((0, PAD), (0, 0))),
        norm_gain[None, :],
    )
    far = flip(mine, 8)
    wg2, wu2 = flip(wg, 1), flip(wu, 1)
    own = jnp.stack([mine, far])
    other = flip(own, 1)
    buf, gain = call(
        dispatch_body, (shape(n, feats), shape(PAD, feats)), 3, True, 150_000_000, 4
    )(pos, place, own, other)

    def mix(which):
        return call(
            functools.partial(mix_body, which), (shape(n, tok),), 2, False, 1_000_000, 4
        )(rows, gate_share.T)

    (high,) = mix(0)
    here = lax.all_to_all(
        buf.reshape(n_ep, half, feats), EP, split_axis=0, concat_axis=0, tiled=True
    ).reshape(n, feats)
    sent = jnp.concatenate([here, gain], axis=0)
    left = step(sent, 1)
    right = step(sent, -1)
    wd2 = flip(wd, 1)
    wide = shape(n, 2 * hid, dtype=F32)
    slim = shape(n, hid, dtype=F32)
    thin = shape(n, 128, dtype=F32)
    gate, up, squares = call(near_body, (slim, slim, thin), 4, True, 300_000_000, 6)(
        pos, here, gain, wg, wu
    )
    left, right, gate = lax.optimization_barrier((left, right, gate))
    left2 = step(left[:h], 1)
    right2 = step(right[h:], -1)
    gate, up, squares = call(
        middle_body, (wide, wide, thin), 11, True, 1_300_000_000, 10
    )(pos, here, gain, left, right, gate, up, squares, wg, wu, wg2, wu2)
    send_a, send_b, hidden = call(
        far_body, (shape(h, feats), shape(h, feats), shape(n, 2 * hid)), 11, True, 800_000_000, 10
    )(pos, left2, right2, gate, up, squares, wg, wu, wg2, wu2, wd, wd2)
    got_a = step(send_a, 1)
    got_b = step(send_b, -1)
    whole = shape(n, feats)
    to_left, keep, to_right = call(
        keep_body, (whole, whole, whole), 3, True, 800_000_000, 6
    )(pos, hidden, wd, wd2)
    to_left, to_right = call(relay_body, (whole, whole), 4, False, 1_000_000, 4)(
        to_left, to_right, got_a, got_b
    )
    from_left = step(to_right, 1)
    from_right = step(to_left, -1)
    (sums,) = call(add_body, (whole,), 3, False, 1_000_000, 4)(keep, from_left, from_right)
    returned = lax.all_to_all(
        sums.reshape(n_ep, half, feats), EP, split_axis=0, concat_axis=0, tiled=True
    ).reshape(n, feats)
    (low,) = mix(1)
    part = shape(2, tok, width, dtype=F32)
    own, away = call(combine_body, (part, part), 3, True, 300_000_000, 6)(pos, high, low, returned)
    near, far = call(
        fold_body, (shape(tok, width, dtype=F32), shape(tok, width)), 2, False, 1_000_000, 2
    )(own, flip(away, 1))
    return (near + flip(far, 8).astype(F32)).astype(BF16)


def solution(mesh):
    n_ep, n_tp = mesh.devices.shape
    side = 8 if n_ep == 64 else n_ep
    fine = Mesh(
        mesh.devices.reshape(n_ep // side, side, 2, n_tp // 4, 2), ("z", "y", "g", "r", "c")
    )
    tp = TP
    in_specs = (
        P(EP, tp),
        P(tp),
        P(EP, None),
        P(EP, None),
        P(EP, None, tp),
        P(EP, None, tp),
        P(EP, tp, None),
    )
    return jax.shard_map(shards, mesh=fine, in_specs=in_specs, out_specs=P(EP, tp), check_vma=False)
```

```python
import functools

import jax
import jax.numpy as jnp
from jax import lax
from jax.experimental import pallas as pl
from jax.experimental.pallas import tpu as pltpu
from jax.sharding import Mesh, PartitionSpec as P

EPS = 1e-06
PAD = 16
EP = ("z", "y")
X = ("g", "r")
TP = ("g", "r", "c")
F32 = jnp.float32
BF16 = jnp.bfloat16
INTERPRET = False


def vmem(n):
    return [pl.BlockSpec(memory_space=pltpu.VMEM)] * n


SMEM = pl.BlockSpec(memory_space=pltpu.SMEM)


def call(body, outs, n_in, scalar, flops, mib):
    return pl.pallas_call(
        body,
        out_shape=outs,
        in_specs=([SMEM] if scalar else []) + vmem(n_in),
        out_specs=tuple(vmem(len(outs))),
        cost_estimate=pl.CostEstimate(flops=flops, bytes_accessed=4 << 20, transcendentals=0),
        compiler_params=pltpu.CompilerParams(vmem_limit_bytes=mib << 20),
        interpret=INTERPRET,
    )


def slots_body(experts, pos, ids, rows, place):
    tok = ids.shape[1]
    half = place.shape[0] // experts
    e_iota = lax.broadcasted_iota(jnp.int32, (experts, tok), 0)
    hit = [e_iota == ids[k : k + 1, :] for k in range(2)]
    named = (hit[0] | hit[1]).astype(F32).astype(BF16)
    before = lax.broadcasted_iota(jnp.int32, (tok, tok), 0) < lax.broadcasted_iota(
        jnp.int32, (tok, tok), 1
    )
    counts = jnp.dot(named, before.astype(F32).astype(BF16), preferred_element_type=F32)
    r_iota = lax.broadcasted_iota(jnp.int32, place.shape, 0)
    here = None
    for k in range(2):
        slot = jnp.sum(jnp.where(hit[k], counts, 0.0), axis=0, keepdims=True).astype(jnp.int32)
        slot = slot - pos[0] * half
        row = jnp.where((slot >= 0) & (slot < half), ids[k : k + 1, :] * half + slot, -1)
        rows[k : k + 1, :] = row
        match = r_iota == row
        here = match if here is None else here | match
    place[...] = here.astype(F32).astype(BF16)


def dispatch_body(pos, place, own, other, buf, gain):
    tok = place.shape[1]
    low = pos[0] == 0
    for s in range(2):
        group = pos[1] if s == 0 else 1 - pos[1]
        cols = pl.ds(pl.multiple_of(group * 256, 256), 256)
        a = own[s]
        b = other[s]
        x = jnp.concatenate([jnp.where(low, a, b), jnp.where(low, b, a)], axis=1)
        buf[:, cols] = jnp.dot(place[...], x[:tok], preferred_element_type=F32).astype(BF16)
        gain[:, cols] = x[tok:]


def product(x, quarter, w):
    k = x.shape[1]
    return jnp.dot(x, w[:, pl.ds(quarter, 1)].reshape(k, w.shape[3]), preferred_element_type=F32)


def near_body(pos, mine, gain, wg, wu, gate, up, squares):
    x = mine[...].astype(F32)
    squares[...] = jnp.broadcast_to(jnp.sum(x * x, axis=1, keepdims=True), squares.shape)
    y = (x * gain[0:1, :].astype(F32)).astype(BF16)
    gate[...] = product(y, pos[2], wg)
    up[...] = product(y, pos[2], wu)


def middle_body(
    pos, mine, gain_m, left, right, gate_in, up_in, squares_in, wg, wu, wg2, wu2, gate, up, squares
):
    n = mine.shape[0]
    total = squares_in[...]
    ys = []
    for piece in (left, right):
        x = piece[:n].astype(F32)
        total = total + jnp.sum(x * x, axis=1, keepdims=True)
        ys.append((x * piece[n : n + 1, :].astype(F32)).astype(BF16))
    squares[...] = total
    y = (mine[...].astype(F32) * gain_m[0:1, :].astype(F32)).astype(BF16)
    ql = (pos[2] + 3) % 4
    qr = (pos[2] + 1) % 4
    hid = wg.shape[3]
    for w, start, out in ((wg, gate_in, gate), (wu, up_in, up)):
        out[:, :hid] = start[...] + (product(ys[0], ql, w) + product(ys[1], qr, w))
    for w, out in ((wg2, gate), (wu2, up)):
        out[:, hid:] = product(y, pos[2], w) + (product(ys[0], ql, w) + product(ys[1], qr, w))


def far_body(
    pos, left2, right2, gate, up, squares, wg, wu, wg2, wu2, wd, wd2, send_a, send_b, hidden
):
    h = left2.shape[0]
    x = jnp.concatenate([left2[...], right2[:h]], axis=0).astype(F32)
    total = squares[:, 0:1] + jnp.sum(x * x, axis=1, keepdims=True)
    factor = lax.rsqrt(total / (4 * x.shape[1]) + EPS)
    y = (x * right2[h : h + 1, :].astype(F32)).astype(BF16)
    hid = wg.shape[3]
    quarter = (pos[2] + 2) % 4
    for i, (w_gate, w_up) in enumerate(((wg, wu), (wg2, wu2))):
        cols = slice(i * hid, (i + 1) * hid)
        g = (gate[:, cols] + product(y, quarter, w_gate)) * factor
        u = (up[:, cols] + product(y, quarter, w_up)) * factor
        hidden[:, cols] = (g / (1.0 + jnp.exp(-g)) * u).astype(BF16)
    down(hidden[...], wd, wd2, quarter, (send_a, send_b))


def down(hid, wd, wd2, quarter, outs):
    k = wd.shape[0]
    rows = hid.shape[0] // len(outs)
    for g in range(2):
        cols = pl.ds(pl.multiple_of(g * 1024 + quarter * 256, 256), 256)
        y = (
            jnp.dot(hid[:, :k], wd[:, cols], preferred_element_type=F32)
            + jnp.dot(hid[:, k:], wd2[:, cols], preferred_element_type=F32)
        ).astype(BF16)
        for i, out in enumerate(outs):
            out[:, g * 256 : (g + 1) * 256] = y[i * rows : (i + 1) * rows]


def keep_body(pos, hidden, wd, wd2, to_left, keep, to_right):
    hid = hidden[...]
    down(hid, wd, wd2, (pos[2] + 3) % 4, (to_left,))
    down(hid, wd, wd2, pos[2], (keep,))
    down(hid, wd, wd2, (pos[2] + 1) % 4, (to_right,))


def relay_body(to_left, to_right, got_a, got_b, left, right):
    h = got_a.shape[0]
    right[:h] = (to_right[:h].astype(F32) + got_a[...].astype(F32)).astype(BF16)
    right[h:] = to_right[h:]
    left[:h] = to_left[:h]
    left[h:] = (to_left[h:].astype(F32) + got_b[...].astype(F32)).astype(BF16)


def add_body(keep, got_a, got_b, out):
    out[...] = (
        keep[...].astype(F32) + got_a[...].astype(F32) + got_b[...].astype(F32)
    ).astype(BF16)


def mix_body(rows, share, high, low):
    r_iota = lax.broadcasted_iota(jnp.int32, high.shape, 0)
    weight = jnp.zeros(high.shape, F32)
    for k in range(2):
        weight = jnp.where(r_iota == rows[k : k + 1, :], share[k : k + 1, :], weight)
    top = weight.astype(BF16)
    high[...] = top
    low[...] = (weight - top.astype(F32)).astype(BF16)


def combine_body(pos, high, low, back, own, away):
    dims = (((0,), (0,)), ((), ()))
    first = pos[0] == 0
    for s in range(2):
        group = pos[1] if s == 0 else 1 - pos[1]
        x = back[:, pl.ds(pl.multiple_of(group * 256, 256), 256)]
        y = lax.dot_general(high[...], x, dims, preferred_element_type=F32) + lax.dot_general(
            low[...], x, dims, preferred_element_type=F32
        )
        a = y[:, :128]
        b = y[:, 128:]
        own[s] = jnp.where(first, a, b)
        away[s] = jnp.where(first, b, a)


def fold_body(own, got, near, far):
    far[...] = (own[1] + got[1]).astype(BF16)
    near[...] = own[0] + got[0]


def shards(tokens, norm_gain, expert_ids, gate_share, gate_weight, up_weight, down_weight):
    tok, width = tokens.shape
    n_ep = lax.axis_size("z") * lax.axis_size("y")
    slot_cap = 4 * tok // n_ep
    half = slot_cap // 2
    n = n_ep * half
    h = n // 2
    feats = 4 * width
    pos = jnp.stack([lax.axis_index("c"), lax.axis_index("g"), lax.axis_index("r")])
    pos = pos.astype(jnp.int32)

    def step(x, s):
        return lax.ppermute(x, X, [(i, (i + s) % 8) for i in range(8)])

    def flip(x, bits):
        return lax.ppermute(x, TP, [(i, i ^ bits) for i in range(16)])

    hid = gate_weight.shape[2]
    wg = gate_weight.reshape(2, 4, 256, hid)
    wu = up_weight.reshape(2, 4, 256, hid)
    wd = down_weight.reshape(hid, down_weight.shape[2])

    def shape(*dims, dtype=BF16):
        return jax.ShapeDtypeStruct(dims, dtype)

    rows, place = call(
        functools.partial(slots_body, n_ep),
        (shape(2, tok, dtype=jnp.int32), shape(n, tok)),
        1,
        True,
        20_000_000,
        4,
    )(pos, expert_ids.T)
    mine = jnp.where(
        lax.broadcasted_iota(jnp.int32, (tok + PAD, width), 0) < tok,
        jnp.pad(tokens, ((0, PAD), (0, 0))),
        norm_gain[None, :],
    )
    own = jnp.stack([mine, flip(mine, 8)])
    other = flip(own, 1)
    buf, gain = call(
        dispatch_body, (shape(n, feats), shape(PAD, feats)), 3, True, 150_000_000, 4
    )(pos, place, own, other)
    here = lax.all_to_all(
        buf.reshape(n_ep, half, feats), EP, split_axis=0, concat_axis=0, tiled=True
    ).reshape(n, feats)
    sent = jnp.concatenate([here, gain], axis=0)
    left = step(sent, 1)
    right = step(sent, -1)
    left2 = step(sent[:h], 2)
    right2 = step(sent[h:], -2)
    wg2, wu2, wd2 = flip(wg, 1), flip(wu, 1), flip(wd, 1)
    wide = shape(n, 2 * hid, dtype=F32)
    slim = shape(n, hid, dtype=F32)
    thin = shape(n, 128, dtype=F32)
    gate, up, squares = call(near_body, (slim, slim, thin), 4, True, 300_000_000, 6)(
        pos, here, gain, wg, wu
    )
    gate, up, squares = call(
        middle_body, (wide, wide, thin), 11, True, 1_300_000_000, 10
    )(pos, here, gain, left, right, gate, up, squares, wg, wu, wg2, wu2)
    send_a, send_b, hidden = call(
        far_body, (shape(h, feats), shape(h, feats), shape(n, 2 * hid)), 11, True, 800_000_000, 10
    )(pos, left2, right2, gate, up, squares, wg, wu, wg2, wu2, wd, wd2)
    got_a = step(send_a, 1)
    got_b = step(send_b, -1)
    whole = shape(n, feats)
    to_left, keep, to_right = call(
        keep_body, (whole, whole, whole), 3, True, 800_000_000, 6
    )(pos, hidden, wd, wd2)
    to_left, to_right = call(relay_body, (whole, whole), 4, False, 1_000_000, 4)(
        to_left, to_right, got_a, got_b
    )
    from_left = step(to_right, 1)
    from_right = step(to_left, -1)
    (sums,) = call(add_body, (whole,), 3, False, 1_000_000, 4)(keep, from_left, from_right)
    returned = lax.all_to_all(
        sums.reshape(n_ep, half, feats), EP, split_axis=0, concat_axis=0, tiled=True
    ).reshape(n, feats)
    high, low = call(mix_body, (shape(n, tok), shape(n, tok)), 2, False, 1_000_000, 4)(
        rows, gate_share.T
    )
    part = shape(2, tok, width, dtype=F32)
    own, away = call(combine_body, (part, part), 3, True, 300_000_000, 6)(pos, high, low, returned)
    near, far = call(
        fold_body, (shape(tok, width, dtype=F32), shape(tok, width)), 2, False, 1_000_000, 2
    )(own, flip(away, 1))
    return (near + flip(far, 8).astype(F32)).astype(BF16)


def solution(mesh):
    n_ep, n_tp = mesh.devices.shape
    side = 8 if n_ep == 64 else n_ep
    fine = Mesh(
        mesh.devices.reshape(n_ep // side, side, 2, n_tp // 4, 2), ("z", "y", "g", "r", "c")
    )
    tp = TP
    in_specs = (
        P(EP, tp),
        P(tp),
        P(EP, None),
        P(EP, None),
        P(EP, None, tp),
        P(EP, None, tp),
        P(EP, tp, None),
    )
    return jax.shard_map(shards, mesh=fine, in_specs=in_specs, out_specs=P(EP, tp), check_vma=False)
```

```python
import functools

import jax
import jax.numpy as jnp
from jax import lax
from jax.experimental import pallas as pl
from jax.experimental.pallas import tpu as pltpu
from jax.sharding import Mesh, PartitionSpec as P

EPS = 1e-06
PAD = 16
EP = ("z", "y")
X = ("g", "r")
TP = ("g", "r", "c")
F32 = jnp.float32
BF16 = jnp.bfloat16
INTERPRET = False


def vmem(n):
    return [pl.BlockSpec(memory_space=pltpu.VMEM)] * n


SMEM = pl.BlockSpec(memory_space=pltpu.SMEM)


def call(body, outs, n_in, scalar, flops, mib):
    return pl.pallas_call(
        body,
        out_shape=outs,
        in_specs=([SMEM] if scalar else []) + vmem(n_in),
        out_specs=tuple(vmem(len(outs))),
        cost_estimate=pl.CostEstimate(flops=flops, bytes_accessed=4 << 20, transcendentals=0),
        compiler_params=pltpu.CompilerParams(vmem_limit_bytes=mib << 20),
        interpret=INTERPRET,
    )


def slots_body(experts, pos, ids, rows, place):
    tok = ids.shape[1]
    half = place.shape[0] // experts
    e_iota = lax.broadcasted_iota(jnp.int32, (experts, tok), 0)
    hit = [e_iota == ids[k : k + 1, :] for k in range(2)]
    named = (hit[0] | hit[1]).astype(F32).astype(BF16)
    before = lax.broadcasted_iota(jnp.int32, (tok, tok), 0) < lax.broadcasted_iota(
        jnp.int32, (tok, tok), 1
    )
    counts = jnp.dot(named, before.astype(F32).astype(BF16), preferred_element_type=F32)
    r_iota = lax.broadcasted_iota(jnp.int32, place.shape, 0)
    here = None
    for k in range(2):
        slot = jnp.sum(jnp.where(hit[k], counts, 0.0), axis=0, keepdims=True).astype(jnp.int32)
        slot = slot - pos[0] * half
        row = jnp.where((slot >= 0) & (slot < half), ids[k : k + 1, :] * half + slot, -1)
        rows[k : k + 1, :] = row
        match = r_iota == row
        here = match if here is None else here | match
    place[...] = here.astype(F32).astype(BF16)


def dispatch_body(pos, place, own, other, buf, gain):
    tok = place.shape[1]
    low = pos[0] == 0
    for s in range(2):
        group = pos[1] if s == 0 else 1 - pos[1]
        cols = pl.ds(pl.multiple_of(group * 256, 256), 256)
        a = own[s]
        b = other[s]
        x = jnp.concatenate([jnp.where(low, a, b), jnp.where(low, b, a)], axis=1)
        buf[:, cols] = jnp.dot(place[...], x[:tok], preferred_element_type=F32).astype(BF16)
        gain[:, cols] = x[tok:]


def product(x, quarter, w):
    k = x.shape[1]
    return jnp.dot(x, w[:, pl.ds(quarter, 1)].reshape(k, w.shape[3]), preferred_element_type=F32)


def near_body(pos, mine, gain, wg, wu, gate, up, squares):
    x = mine[...].astype(F32)
    squares[...] = jnp.broadcast_to(jnp.sum(x * x, axis=1, keepdims=True), squares.shape)
    y = (x * gain[0:1, :].astype(F32)).astype(BF16)
    gate[...] = product(y, pos[2], wg)
    up[...] = product(y, pos[2], wu)


def middle_body(
    pos, mine, gain_m, left, right, gate_in, up_in, squares_in, wg, wu, wg2, wu2, gate, up, squares
):
    n = mine.shape[0]
    total = squares_in[...]
    ys = []
    for piece in (left, right):
        x = piece[:n].astype(F32)
        total = total + jnp.sum(x * x, axis=1, keepdims=True)
        ys.append((x * piece[n : n + 1, :].astype(F32)).astype(BF16))
    squares[...] = total
    y = (mine[...].astype(F32) * gain_m[0:1, :].astype(F32)).astype(BF16)
    ql = (pos[2] + 3) % 4
    qr = (pos[2] + 1) % 4
    hid = wg.shape[3]
    for w, start, out in ((wg, gate_in, gate), (wu, up_in, up)):
        out[:, :hid] = start[...] + (product(ys[0], ql, w) + product(ys[1], qr, w))
    for w, out in ((wg2, gate), (wu2, up)):
        out[:, hid:] = product(y, pos[2], w) + (product(ys[0], ql, w) + product(ys[1], qr, w))


def far_body(
    pos, left2, right2, gate, up, squares, wg, wu, wg2, wu2, wd, wd2, send_a, send_b, hidden
):
    h = left2.shape[0]
    x = jnp.concatenate([left2[...], right2[:h]], axis=0).astype(F32)
    total = squares[:, 0:1] + jnp.sum(x * x, axis=1, keepdims=True)
    factor = lax.rsqrt(total / (4 * x.shape[1]) + EPS)
    y = (x * right2[h : h + 1, :].astype(F32)).astype(BF16)
    hid = wg.shape[3]
    quarter = (pos[2] + 2) % 4
    for i, (w_gate, w_up) in enumerate(((wg, wu), (wg2, wu2))):
        cols = slice(i * hid, (i + 1) * hid)
        g = (gate[:, cols] + product(y, quarter, w_gate)) * factor
        u = (up[:, cols] + product(y, quarter, w_up)) * factor
        hidden[:, cols] = (g / (1.0 + jnp.exp(-g)) * u).astype(BF16)
    down(hidden[...], wd, wd2, quarter, (send_a, send_b))


def down(hid, wd, wd2, quarter, outs):
    k = wd.shape[0]
    rows = hid.shape[0] // len(outs)
    for g in range(2):
        cols = pl.ds(pl.multiple_of(g * 1024 + quarter * 256, 256), 256)
        y = (
            jnp.dot(hid[:, :k], wd[:, cols], preferred_element_type=F32)
            + jnp.dot(hid[:, k:], wd2[:, cols], preferred_element_type=F32)
        ).astype(BF16)
        for i, out in enumerate(outs):
            out[:, g * 256 : (g + 1) * 256] = y[i * rows : (i + 1) * rows]


def keep_body(pos, hidden, wd, wd2, to_left, keep, to_right):
    hid = hidden[...]
    down(hid, wd, wd2, (pos[2] + 3) % 4, (to_left,))
    down(hid, wd, wd2, pos[2], (keep,))
    down(hid, wd, wd2, (pos[2] + 1) % 4, (to_right,))


def relay_body(to_left, to_right, got_a, got_b, left, right):
    h = got_a.shape[0]
    right[:h] = (to_right[:h].astype(F32) + got_a[...].astype(F32)).astype(BF16)
    right[h:] = to_right[h:]
    left[:h] = to_left[:h]
    left[h:] = (to_left[h:].astype(F32) + got_b[...].astype(F32)).astype(BF16)


def add_body(keep, got_a, got_b, out):
    out[...] = (
        keep[...].astype(F32) + got_a[...].astype(F32) + got_b[...].astype(F32)
    ).astype(BF16)


def mix_body(rows, share, high, low):
    r_iota = lax.broadcasted_iota(jnp.int32, high.shape, 0)
    weight = jnp.zeros(high.shape, F32)
    for k in range(2):
        weight = jnp.where(r_iota == rows[k : k + 1, :], share[k : k + 1, :], weight)
    top = weight.astype(BF16)
    high[...] = top
    low[...] = (weight - top.astype(F32)).astype(BF16)


def combine_body(pos, high, low, back, own, away):
    dims = (((0,), (0,)), ((), ()))
    first = pos[0] == 0
    for s in range(2):
        group = pos[1] if s == 0 else 1 - pos[1]
        x = back[:, pl.ds(pl.multiple_of(group * 256, 256), 256)]
        y = lax.dot_general(high[...], x, dims, preferred_element_type=F32) + lax.dot_general(
            low[...], x, dims, preferred_element_type=F32
        )
        a = y[:, :128]
        b = y[:, 128:]
        own[s] = jnp.where(first, a, b)
        away[s] = jnp.where(first, b, a)


def fold_body(own, got, near, far):
    far[...] = (own[1] + got[1]).astype(BF16)
    near[...] = own[0] + got[0]


def shards(tokens, norm_gain, expert_ids, gate_share, gate_weight, up_weight, down_weight):
    tok, width = tokens.shape
    n_ep = lax.axis_size("z") * lax.axis_size("y")
    slot_cap = 4 * tok // n_ep
    half = slot_cap // 2
    n = n_ep * half
    h = n // 2
    feats = 4 * width
    pos = jnp.stack([lax.axis_index("c"), lax.axis_index("g"), lax.axis_index("r")])
    pos = pos.astype(jnp.int32)

    def step(x, s):
        return lax.ppermute(x, X, [(i, (i + s) % 8) for i in range(8)])

    def flip(x, bits):
        return lax.ppermute(x, TP, [(i, i ^ bits) for i in range(16)])

    hid = gate_weight.shape[2]
    wg = gate_weight.reshape(2, 4, 256, hid)
    wu = up_weight.reshape(2, 4, 256, hid)
    wd = down_weight.reshape(hid, down_weight.shape[2])

    def shape(*dims, dtype=BF16):
        return jax.ShapeDtypeStruct(dims, dtype)

    rows, place = call(
        functools.partial(slots_body, n_ep),
        (shape(2, tok, dtype=jnp.int32), shape(n, tok)),
        1,
        True,
        20_000_000,
        4,
    )(pos, expert_ids.T)
    mine = jnp.where(
        lax.broadcasted_iota(jnp.int32, (tok + PAD, width), 0) < tok,
        jnp.pad(tokens, ((0, PAD), (0, 0))),
        norm_gain[None, :],
    )
    own = jnp.stack([mine, flip(mine, 8)])
    other = flip(own, 1)
    buf, gain = call(
        dispatch_body, (shape(n, feats), shape(PAD, feats)), 3, True, 150_000_000, 4
    )(pos, place, own, other)
    here = lax.all_to_all(
        buf.reshape(n_ep, half, feats), EP, split_axis=0, concat_axis=0, tiled=True
    ).reshape(n, feats)
    sent = jnp.concatenate([here, gain], axis=0)
    left = step(sent, 1)
    right = step(sent, -1)
    wg2, wu2, wd2 = flip(wg, 1), flip(wu, 1), flip(wd, 1)
    wide = shape(n, 2 * hid, dtype=F32)
    slim = shape(n, hid, dtype=F32)
    thin = shape(n, 128, dtype=F32)
    gate, up, squares = call(near_body, (slim, slim, thin), 4, True, 300_000_000, 6)(
        pos, here, gain, wg, wu
    )
    left, right, gate = lax.optimization_barrier((left, right, gate))
    left2 = step(left[:h], 1)
    right2 = step(right[h:], -1)
    gate, up, squares = call(
        middle_body, (wide, wide, thin), 11, True, 1_300_000_000, 10
    )(pos, here, gain, left, right, gate, up, squares, wg, wu, wg2, wu2)
    send_a, send_b, hidden = call(
        far_body, (shape(h, feats), shape(h, feats), shape(n, 2 * hid)), 11, True, 800_000_000, 10
    )(pos, left2, right2, gate, up, squares, wg, wu, wg2, wu2, wd, wd2)
    got_a = step(send_a, 1)
    got_b = step(send_b, -1)
    whole = shape(n, feats)
    to_left, keep, to_right = call(
        keep_body, (whole, whole, whole), 3, True, 800_000_000, 6
    )(pos, hidden, wd, wd2)
    to_left, to_right = call(relay_body, (whole, whole), 4, False, 1_000_000, 4)(
        to_left, to_right, got_a, got_b
    )
    from_left = step(to_right, 1)
    from_right = step(to_left, -1)
    (sums,) = call(add_body, (whole,), 3, False, 1_000_000, 4)(keep, from_left, from_right)
    returned = lax.all_to_all(
        sums.reshape(n_ep, half, feats), EP, split_axis=0, concat_axis=0, tiled=True
    ).reshape(n, feats)
    high, low = call(mix_body, (shape(n, tok), shape(n, tok)), 2, False, 1_000_000, 4)(
        rows, gate_share.T
    )
    part = shape(2, tok, width, dtype=F32)
    own, away = call(combine_body, (part, part), 3, True, 300_000_000, 6)(pos, high, low, returned)
    near, far = call(
        fold_body, (shape(tok, width, dtype=F32), shape(tok, width)), 2, False, 1_000_000, 2
    )(own, flip(away, 1))
    return (near + flip(far, 8).astype(F32)).astype(BF16)


def solution(mesh):
    n_ep, n_tp = mesh.devices.shape
    side = 8 if n_ep == 64 else n_ep
    fine = Mesh(
        mesh.devices.reshape(n_ep // side, side, 2, n_tp // 4, 2), ("z", "y", "g", "r", "c")
    )
    tp = TP
    in_specs = (
        P(EP, tp),
        P(tp),
        P(EP, None),
        P(EP, None),
        P(EP, None, tp),
        P(EP, None, tp),
        P(EP, tp, None),
    )
    return jax.shard_map(shards, mesh=fine, in_specs=in_specs, out_specs=P(EP, tp), check_vma=False)
```
